512 devices in a mesh: ep: 32 (over z, core), tp: 16 (over y, x).
Axes of the slice: x: 4, y: 4, z: 16, core: 2. Of those that a mesh axis runs over, the one named last changes fastest.
Arguments:
- mixer_input: bfloat16 [4096, 2048], P('ep'), may hold values from -6 to 6
- mixer_gain: float32 [2048], replicated, may hold values from 0.1 to 1.9
- glu_value_weight: bfloat16 [512, 2048], P('tp'), may hold values from -0.125 to 0.125
- glu_gate_weight: bfloat16 [512, 2048], P('tp'), may hold values from -0.125 to 0.125
- conv_taps: float32 [512, 31], P('tp'), may hold values from -1 to 1
- conv_bias: float32 [512], P('tp'), may hold values from -3 to 3
- channel_gain: float32 [512], replicated, may hold values from 0.1 to 1.9
- channel_shift: float32 [512], replicated, may hold values from -3 to 3
- mixer_out_weight: bfloat16 [512, 2048], P(None, 'tp'), may hold values from -0.25 to 0.25
- expert_input: bfloat16 [8192, 2048], P('ep'), may hold values from -6 to 6
- expert_gain: float32 [2048], replicated, may hold values from 0.1 to 1.9
- routes: int32 [8192, 2], P('ep'), may hold values from 0 to 31, all different within a row; in each aligned block of 256 rows (0 to 255, 256 to 511, ...) at most 24 rows name the same one
- route_logits: float32 [8192, 2], P('ep'), may hold values from -8 to 8
- gate_weight: bfloat16 [32, 2048, 4096], P('ep', None, 'tp'), may hold values from -0.125 to 0.125
- up_weight: bfloat16 [32, 2048, 4096], P('ep', None, 'tp'), may hold values from -0.125 to 0.125
- down_weight: bfloat16 [32, 4096, 2048], P('ep', 'tp'), may hold values from -0.09375 to 0.09375
Outputs:
- mixer_output: bfloat16 [4096, 2048], P('ep', 'tp')
- expert_output: bfloat16 [8192, 2048], P('ep', 'tp')
The draws below stay inside these ranges and needn't reach their ends.
Inputs may be any that keep to these rules, and one draw needn't show every extreme that they name: `routes`: the 2 entries of a row differ. Among the rows of one index of ep, no expert is named by more than 24 rows, a bound that some block reaches.
All inputs are finite; a program needn't handle non-finite values.
Results may differ from the reference program's by a relative error of at most 0.015.
Values may be sent and summed in bfloat16 or wider, within the bound.
No kernel may reach another device: no remote copies, remote signals or barrier semaphores. Data moves between devices by JAX's collectives and lax.ppermute only.
A program may use at most 64 MiB of HBM per device.

```python
import math
import jax
import jax.numpy as jnp
import numpy as np
from jax import lax

D = 2048
CH = 512
FF = 4096
KERNEL = 31
TOP = 2
ROWS_B = 256
EXPERTS = 32
CAP = 24
TOKENS_A = 4096
TOKENS_B = 8192
N_EP = 32
N_TP = 16


def shard_levels(own_key, extent, pieces, least, high):
    def one(axis_at, blocks):
        steps = jax.random.uniform(jax.random.fold_in(jax.random.fold_in(own_key, 6), axis_at), (blocks,), jnp.float32, least / len(pieces), high / len(pieces))
        return jnp.repeat(jnp.exp(steps), extent[axis_at] // blocks).reshape((-1,) + (1,) * (len(extent) - axis_at - 1))

    factor_of = one(*pieces[0])
    for cut in pieces[1:]:
        factor_of = factor_of * one(*cut)
    return factor_of


def assign_block(rng, own, number, rows, count, top, limit, skew):
    order = jax.random.permutation(rng, count)
    crowded, usual = portions_of(count, rows * top, limit, skew, True), portions_of(count, rows * top, limit, skew, False)
    places = jnp.arange(count)

    def named(sizes, rotation):
        used = int((sizes > 0).sum())
        fixed = max(1, used // 4)
        moved = fixed + (places - fixed + rotation * (used - fixed)) % max(1, count - fixed)
        return jnp.zeros((count,), jnp.int32).at[order[jnp.where(places < fixed, places, moved)]].set(jnp.asarray(sizes, jnp.int32))

    sizes = jnp.where(number % 4 == 0, named(crowded, number // 4), named(usual, number - number // 4 - 1))
    mixed = jax.random.permutation(jax.random.fold_in(own, 3), count)
    giver, sink = mixed[0:count // 2 * 2:2], mixed[1:count // 2 * 2:2]
    room = jnp.minimum(sizes[giver] - 1, limit - sizes[sink]) // 2
    room = jnp.where((giver == order[0]) | (sink == order[0]) | (sizes[sink] == 0), 0, jnp.maximum(room, 0))
    moved = jax.random.randint(jax.random.fold_in(own, 4), (count // 2,), 0, 1 << 20) % (room + 1)
    sizes = sizes.at[giver].add(-moved).at[sink].add(moved)
    labels = jnp.searchsorted(jnp.cumsum(sizes), jnp.arange(rows * top), side="right").astype(jnp.int32)
    listing = labels.reshape(top, rows).T
    listing = listing[jax.random.permutation(jax.random.fold_in(own, 1), rows)]
    rotation = jax.random.randint(jax.random.fold_in(own, 2), (rows, 1), 0, top)
    return jnp.take_along_axis(listing, (jnp.arange(top)[None, :] + rotation) % top, axis=1)


def portions_of(number_of, total, most, lean, full):
    portions = [(1 << 20) // math.isqrt(grade ** lean) + 1 for grade in range(1, number_of + 1)]
    largest = most if full else min(most, max(-(-total // number_of), total * portions[0] // sum(portions)))
    least = 1 if total - largest >= number_of - 1 else 0
    counts, surplus = [largest] + [least] * (number_of - 1), total - largest - least * (number_of - 1)
    while surplus > 0:
        free = [i for i in range(1, number_of) if counts[i] < largest] or [i for i in range(1, number_of) if counts[i] < most]
        pool, budget = sum([portions[i] for i in free]), surplus
        for i in free:
            extra = min(most - counts[i], max(1, budget * portions[i] // pool), surplus)
            counts[i] = counts[i] + extra
            surplus = surplus - extra
    return np.array(counts)


def noise(rng, dims, width, reach, split=(), kind=jnp.bfloat16):
    array = jax.random.normal(rng, dims, jnp.float32) * width
    if len(split) > 0:
        array = shard_levels(rng, dims, split, -0.22, 0.18) * array
    return jnp.clip(array, min=-reach, max=reach).astype(kind)


def setup_inputs(seed: int = 0) -> dict:
    key_list = jax.random.split(jax.random.key(seed), 17)
    mixer_input = noise(key_list[0], (TOKENS_A, D), 1.0, 6.0, ((0, 32),))
    mixer_gain = jnp.clip(1.0 + 0.18 * jax.random.normal(key_list[1], (D,), jnp.float32), 0.1, 1.9)
    glu_value_weight = noise(key_list[2], (CH, D), D ** -0.5, 0.125, ((0, 16),))
    glu_gate_weight = noise(key_list[3], (CH, D), D ** -0.5, 0.125, ((0, 16),))
    conv_taps = noise(key_list[4], (CH, KERNEL), KERNEL ** -0.5, 1.0, ((0, 16),), jnp.float32)
    conv_bias = noise(key_list[5], (CH,), 0.5, 3.0, ((0, 16),), jnp.float32)
    channel_gain = jnp.clip(1.0 + 0.18 * jax.random.normal(key_list[6], (CH,), jnp.float32), 0.1, 1.9)
    channel_shift = noise(key_list[7], (CH,), 0.5, 3.0, (), jnp.float32)
    mixer_out_weight = noise(key_list[8], (CH, D), CH ** -0.5, 0.25, ((1, 16),))
    expert_input = noise(key_list[9], (TOKENS_B, D), 1.0, 6.0, ((0, 32),))
    expert_gain = jnp.clip(1.0 + 0.18 * jax.random.normal(key_list[10], (D,), jnp.float32), 0.1, 1.9)
    routes_keys = jax.random.split(jax.random.fold_in(key_list[11], 1), TOKENS_B // ROWS_B)
    routes_turns = jax.random.permutation(jax.random.fold_in(key_list[11], 3), TOKENS_B // ROWS_B)
    routes = jax.vmap(lambda own, number: assign_block(jax.random.fold_in(key_list[11], 2), own, number, ROWS_B, EXPERTS, TOP, CAP, 1))(routes_keys, routes_turns).reshape((TOKENS_B, TOP))
    route_logits = noise(key_list[12], (TOKENS_B, TOP), 1.5, 8.0, ((0, 32),), jnp.float32)
    gate_weight = noise(key_list[13], (EXPERTS, D, FF), D ** -0.5, 0.125, ((0, 32), (2, 16)))
    up_weight = noise(key_list[14], (EXPERTS, D, FF), D ** -0.5, 0.125, ((0, 32), (2, 16)))
    down_weight = noise(key_list[15], (EXPERTS, FF, D), FF ** -0.5, 0.09375, ((0, 32), (1, 16)))
    return {"mixer_input": mixer_input, "mixer_gain": mixer_gain, "glu_value_weight": glu_value_weight, "glu_gate_weight": glu_gate_weight, "conv_taps": conv_taps, "conv_bias": conv_bias, "channel_gain": channel_gain, "channel_shift": channel_shift, "mixer_out_weight": mixer_out_weight, "expert_input": expert_input, "expert_gain": expert_gain, "routes": routes, "route_logits": route_logits, "gate_weight": gate_weight, "up_weight": up_weight, "down_weight": down_weight}


norm_eps = 1e-06

def rms_rows(row_block, gain_vec):
    row_values = row_block.astype(jnp.float32)
    inv_scale = lax.rsqrt(lax.optimization_barrier(jnp.mean(row_values * row_values, axis=-1, keepdims=True)) + norm_eps)
    return (row_values * inv_scale * gain_vec[None, :]).astype(jnp.bfloat16)

def mixer_half(mixer_input, mixer_gain, glu_value_weight, glu_gate_weight, conv_taps, conv_bias, channel_gain, channel_shift, mixer_out_weight):
    normed = rms_rows(mixer_input, mixer_gain)
    contract = (((1,), (1,)), ((), ()))
    glu_value = lax.dot_general(normed, glu_value_weight, contract, preferred_element_type=jnp.float32)
    glu_gate = lax.dot_general(normed, glu_gate_weight, contract, preferred_element_type=jnp.float32)
    gated_rows = (glu_value * jax.nn.sigmoid(glu_gate)).astype(jnp.bfloat16)
    padded = jnp.pad(gated_rows.astype(jnp.float32), ((KERNEL - 1, 0), (0, 0)))
    conv_sum = jnp.zeros((TOKENS_A, CH), jnp.float32)
    for offset in range(KERNEL):
        conv_sum = conv_sum + padded[offset:offset + TOKENS_A] * conv_taps[:, offset][None, :]
    conv_out = (conv_sum + conv_bias[None, :]).astype(jnp.bfloat16)
    chan_values = conv_out.astype(jnp.float32)
    chan_mean = lax.optimization_barrier(jnp.mean(chan_values, axis=1, keepdims=True))
    centered = chan_values - chan_mean
    variance = lax.optimization_barrier(jnp.mean(centered * centered, axis=1, keepdims=True))
    shaped = centered * lax.rsqrt(variance + norm_eps) * channel_gain[None, :] + channel_shift[None, :]
    activated = jax.nn.silu(shaped).astype(jnp.bfloat16)
    return jnp.dot(activated, mixer_out_weight, preferred_element_type=jnp.float32).astype(jnp.bfloat16)

def expert_half(expert_input, expert_gain, routes, route_logits, gate_weight, up_weight, down_weight):
    normed = rms_rows(expert_input, expert_gain)
    assigned = routes.reshape(N_EP, ROWS_B * TOP)
    matches = (assigned[:, :, None] == jnp.arange(EXPERTS, dtype=jnp.int32)[None, None, :]).astype(jnp.int32)
    earlier = jnp.cumsum(matches, axis=1) - matches
    slot_index = lax.optimization_barrier(jnp.sum(earlier * matches, axis=2))
    source_dev = jnp.arange(N_EP, dtype=jnp.int32)[:, None]
    slot_place = (source_dev * CAP + slot_index).reshape(-1).astype(jnp.int32)
    owner_row = (source_dev * ROWS_B + jnp.arange(ROWS_B * TOP, dtype=jnp.int32)[None, :] // TOP).reshape(-1).astype(jnp.int32)
    expert_ids = assigned.reshape(-1)
    slot_owner = jnp.full((EXPERTS, N_EP * CAP), TOKENS_B, jnp.int32).at[expert_ids, slot_place].set(owner_row)

    def one_expert(packed):
        slot_rows, gate_mat, up_mat, down_mat = packed
        rows_in = jnp.take(normed, slot_rows, axis=0, mode='fill', fill_value=0)
        gate_acts = jnp.dot(rows_in, gate_mat, preferred_element_type=jnp.float32)
        up_acts = jnp.dot(rows_in, up_mat, preferred_element_type=jnp.float32)
        hidden = (jax.nn.silu(gate_acts) * up_acts).astype(jnp.bfloat16)
        hid_groups = hidden.reshape(N_EP * CAP, N_TP, FF // N_TP).astype(jnp.float32)
        down_groups = down_mat.reshape(N_TP, FF // N_TP, D).astype(jnp.float32)
        partial_value = jnp.einsum('sgf,gfd->gsd', hid_groups, down_groups).astype(jnp.bfloat16)
        return lax.optimization_barrier(jnp.sum(partial_value.astype(jnp.float32), axis=0)).astype(jnp.bfloat16)
    results = lax.map(one_expert, (slot_owner, gate_weight, up_weight, down_weight))
    picked = results[expert_ids, slot_place].astype(jnp.float32).reshape(TOKENS_B, TOP, D)
    first_weight = jax.nn.sigmoid(route_logits[:, 0] - route_logits[:, 1])
    second_weight = jax.nn.sigmoid(route_logits[:, 1] - route_logits[:, 0])
    combined = picked[:, 0] * first_weight[:, None] + picked[:, 1] * second_weight[:, None]
    return combined.astype(jnp.bfloat16)

def reference(mixer_input, mixer_gain, glu_value_weight, glu_gate_weight, conv_taps, conv_bias, channel_gain, channel_shift, mixer_out_weight, expert_input, expert_gain, routes, route_logits, gate_weight, up_weight, down_weight):
    mixer_output = mixer_half(mixer_input, mixer_gain, glu_value_weight, glu_gate_weight, conv_taps, conv_bias, channel_gain, channel_shift, mixer_out_weight)
    expert_output = expert_half(expert_input, expert_gain, routes, route_logits, gate_weight, up_weight, down_weight)
    return (mixer_output, expert_output)
```

```python
import jax
import jax.numpy as jnp
from jax import lax
from jax.experimental import pallas as pl
from jax.experimental.pallas import tpu as pltpu
from jax.sharding import PartitionSpec as P

norm_eps = 1e-06
F32 = jnp.float32
BF16 = jnp.bfloat16


def vmem_specs(count):
    return [pl.BlockSpec(memory_space=pltpu.VMEM)] * count


def call(body, outs, *operands):
    return pl.pallas_call(
        body,
        out_shape=tuple(jax.ShapeDtypeStruct(s, d) for s, d in outs),
        in_specs=vmem_specs(len(operands)),
        out_specs=tuple(vmem_specs(len(outs))),
        compiler_params=pltpu.CompilerParams(vmem_limit_bytes=20 * 1024 * 1024),
    )(*operands)


def column_of(row):
    size = row.shape[1]
    at = lax.broadcasted_iota(jnp.int32, (size, size), 0)
    to = lax.broadcasted_iota(jnp.int32, (size, size), 1)
    return jnp.sum(jnp.where(at == to, jnp.broadcast_to(row, (size, size)), 0.0), axis=1, keepdims=True)


def columns_of(row):
    return jnp.transpose(jnp.broadcast_to(row, (8, row.shape[1])))[:, 0:1]


def inv_rms(values):
    return lax.rsqrt(jnp.mean(values * values, axis=-1, keepdims=True) + norm_eps)


def prelude(groups, capacity, width, mix_ref, mgain_ref, wv_ref, wg_ref, exp_ref, egain_ref, routes_ref, logits_ref, out_ref, gated_ref, table_ref):
    rows_b = exp_ref.shape[0]
    routes = routes_ref[...]
    expert = lax.broadcasted_iota(jnp.int32, (groups, rows_b), 0)
    first = expert == routes[0:1, :]
    second = expert == routes[1:2, :]
    named = jnp.where(first | second, 1.0, 0.0)
    before = lax.broadcasted_iota(jnp.int32, (rows_b, rows_b), 0) < lax.broadcasted_iota(jnp.int32, (rows_b, rows_b), 1)
    earlier = jnp.dot(named.astype(BF16), jnp.where(before, 1.0, 0.0).astype(BF16), preferred_element_type=F32)
    slot = expert.astype(F32) * capacity + earlier
    slot_a = jnp.sum(jnp.where(first, slot, 0.0), axis=0, keepdims=True)
    slot_b = jnp.sum(jnp.where(second, slot, 0.0), axis=0, keepdims=True)
    logits = logits_ref[...]
    gap = logits[0:1, :] - logits[1:2, :]
    table_ref[...] = jnp.concatenate([slot_a, slot_b, jax.nn.sigmoid(gap), jax.nn.sigmoid(-gap), jnp.zeros((4, rows_b), F32)], axis=0)
    code = jnp.where(first | second, earlier, -1.0)
    place = lax.broadcasted_iota(jnp.int32, (groups, capacity, rows_b), 1).astype(F32)
    chosen = jnp.where(code[:, None, :] == place, 1.0, 0.0).reshape(groups * capacity, rows_b).astype(BF16)
    scale_b = inv_rms(exp_ref[...].astype(F32))
    start = pl.multiple_of(lax.axis_index("tp") * width, width)
    share = exp_ref[:, pl.ds(start, width)].astype(F32)
    normed_b = (share * scale_b * egain_ref[:, pl.ds(start, width)]).astype(BF16)
    out_ref[...] = jnp.dot(chosen, normed_b, preferred_element_type=F32).astype(BF16)
    rows = mix_ref[...].astype(F32)
    normed_a = (rows * inv_rms(rows) * mgain_ref[...]).astype(BF16)
    nt = (((1,), (1,)), ((), ()))
    value = lax.dot_general(wv_ref[...], normed_a, nt, preferred_element_type=F32)
    gate = lax.dot_general(wg_ref[...], normed_a, nt, preferred_element_type=F32)
    gated_ref[...] = (value * jax.nn.sigmoid(gate)).astype(BF16)


def conv_and_copies(arrived_ref, prev_ref, gated_ref, taps_ref, bias_ref, out_ref):
    count, _, width = out_ref.shape
    slots = arrived_ref.shape[0]
    taps = taps_ref[...]
    reach = taps.shape[1] - 1
    both = jnp.concatenate([prev_ref[...].astype(F32), gated_ref[...].astype(F32)], axis=1)
    span = both.shape[1]
    total = column_of(bias_ref[...]) + taps[:, reach : reach + 1] * both[:, width:]
    for k in range(reach):
        moved = pltpu.roll(both, reach - k, 1)
        total = total + taps[:, k : k + 1] * moved[:, span - width :]
    conv_out = total.astype(BF16)
    arrived = arrived_ref[...]
    for j in range(count):
        out_ref[j, :slots, :] = arrived
        out_ref[j, slots:, :] = conv_out


def experts_and_mixer(slots, block, x_ref, wg_ref, wu_ref, wd_ref, cgain_ref, cshift_ref, wo_ref, out_ref, mix_ref):
    count, _, width = x_ref.shape
    wg, wu, wd = wg_ref[0], wu_ref[0], wd_ref[0]
    for at in range(0, slots, block):
        rows = jnp.concatenate([x_ref[j, at : at + block, :] for j in range(count)], axis=1)
        gate = jnp.dot(rows, wg, preferred_element_type=F32)
        up = jnp.dot(rows, wu, preferred_element_type=F32)
        hidden = (gate * jax.nn.sigmoid(gate) * up).astype(BF16)
        part = jnp.dot(hidden, wd, preferred_element_type=F32).astype(BF16)
        for j in range(count):
            out_ref[j, at : at + block, :] = part[:, j * width : (j + 1) * width]
    values = jnp.concatenate([x_ref[j, slots:, :] for j in range(count)], axis=0).astype(F32)
    centered = values - jnp.mean(values, axis=0, keepdims=True)
    variance = jnp.mean(centered * centered, axis=0, keepdims=True)
    shaped = centered * lax.rsqrt(variance + norm_eps) * columns_of(cgain_ref[...]) + columns_of(cshift_ref[...])
    activated = (shaped * jax.nn.sigmoid(shaped)).astype(BF16)
    mix_ref[...] = lax.dot_general(activated, wo_ref[...], (((0,), (0,)), ((), ())), preferred_element_type=F32).astype(BF16)


def add_parts(parts_ref, out_ref):
    total = parts_ref[0].astype(F32)
    for j in range(1, parts_ref.shape[0]):
        total = total + parts_ref[j].astype(F32)
    out_ref[...] = total.astype(BF16)


def combine(back_ref, table_ref, out_ref):
    rows_b = out_ref.shape[0]
    slots = back_ref.shape[0]
    table = jnp.transpose(table_ref[...])
    place = lax.broadcasted_iota(jnp.int32, (rows_b, slots), 1).astype(F32)
    back = back_ref[...]
    total = None
    for j in range(2):
        pick = jnp.where(table[:, j : j + 1] == place, 1.0, 0.0).astype(BF16)
        term = jnp.dot(pick, back, preferred_element_type=F32) * table[:, 2 + j : 3 + j]
        total = term if total is None else total + term
    out_ref[...] = total.astype(BF16)


def exchange(blocks, axis):
    return lax.all_to_all(blocks, axis, split_axis=0, concat_axis=0, tiled=True)


def on_device(
    mixer_input,
    mixer_gain,
    glu_value_weight,
    glu_gate_weight,
    conv_taps,
    conv_bias,
    channel_gain,
    channel_shift,
    mixer_out_weight,
    expert_input,
    expert_gain,
    routes,
    route_logits,
    gate_weight,
    up_weight,
    down_weight,
):
    groups = lax.axis_size("ep")
    parts = lax.axis_size("tp")
    rows_b, features = expert_input.shape
    width = features // parts
    capacity = 3 * rows_b // groups
    slots = groups * capacity
    channels, tokens = glu_value_weight.shape[0], mixer_input.shape[0]

    def front(*refs):
        prelude(groups, capacity, width, *refs)

    outgoing, gated, table = call(
        front,
        [((slots, width), BF16), ((channels, tokens), BF16), ((8, rows_b), F32)],
        mixer_input,
        mixer_gain[None, :],
        glu_value_weight,
        glu_gate_weight,
        expert_input,
        expert_gain[None, :],
        routes.T,
        route_logits.T,
    )
    before = lax.ppermute(gated, "ep", [(i, i + 1) for i in range(groups - 1)])
    arrived = exchange(outgoing.reshape(groups, capacity, width), "ep").reshape(slots, width)
    (copies,) = call(
        conv_and_copies,
        [((parts, slots + channels, width), BF16)],
        arrived,
        before,
        gated,
        conv_taps,
        conv_bias[None, :],
    )
    gathered = exchange(copies, "tp")

    def middle(*refs):
        experts_and_mixer(slots, 256, *refs)

    partial, mixed = call(
        middle,
        [((parts, slots, width), BF16), ((tokens, width), BF16)],
        gathered,
        gate_weight,
        up_weight,
        down_weight,
        channel_gain[None, :],
        channel_shift[None, :],
        mixer_out_weight,
    )
    (summed,) = call(add_parts, [((slots, width), BF16)], exchange(partial, "tp"))
    returned = exchange(summed.reshape(groups, capacity, width), "ep").reshape(slots, width)
    (combined,) = call(combine, [((rows_b, width), BF16)], returned, table)
    return mixed, combined


def solution(mesh):
    in_specs = (
        P("ep", None),
        P(),
        P("tp", None),
        P("tp", None),
        P("tp", None),
        P("tp"),
        P(),
        P(),
        P(None, "tp"),
        P("ep", None),
        P(),
        P("ep", None),
        P("ep", None),
        P("ep", None, "tp"),
        P("ep", None, "tp"),
        P("ep", "tp", None),
    )
    out_specs = (P("ep", "tp"), P("ep", "tp"))
    return jax.shard_map(
        on_device, mesh=mesh, in_specs=in_specs, out_specs=out_specs, check_vma=False
    )
```

```python
import math

import jax
import jax.numpy as jnp
from jax import lax
from jax.experimental import pallas as pl
from jax.experimental.pallas import tpu as pltpu
from jax.sharding import PartitionSpec as P

norm_eps = 1e-06
F32 = jnp.float32
BF16 = jnp.bfloat16


def whole(space, count):
    return [pl.BlockSpec(memory_space=space)] * count


def call(body, outs, *operands, source=pltpu.VMEM, scratch=()):
    return pl.pallas_call(
        body,
        out_shape=tuple(jax.ShapeDtypeStruct(s, d) for s, d in outs),
        in_specs=whole(source, len(operands)),
        out_specs=tuple(whole(pltpu.VMEM, len(outs))),
        scratch_shapes=list(scratch),
        compiler_params=pltpu.CompilerParams(vmem_limit_bytes=20 * 1024 * 1024),
    )(*operands)


def staged(body, outs, *operands):
    count = len(operands)

    def kernel(*refs):
        sources, results = refs[:count], refs[count : count + len(outs)]
        held, sems = refs[count + len(outs) : -1], refs[-1]
        copies = [pltpu.make_async_copy(sources[i], held[i], sems.at[i]) for i in range(count)]
        for copy in copies:
            copy.start()

        def load(i):
            copies[i].wait()
            return held[i]

        body(load, *results)

    scratch = [pltpu.VMEM(x.shape, x.dtype) for x in operands] + [pltpu.SemaphoreType.DMA((count,))]
    pinned = [pltpu.with_memory_space_constraint(x, pltpu.HBM) for x in operands]
    return call(kernel, outs, *pinned, source=pltpu.HBM, scratch=scratch)


def column_of(row):
    size = row.shape[1]
    at = lax.broadcasted_iota(jnp.int32, (size, size), 0)
    to = lax.broadcasted_iota(jnp.int32, (size, size), 1)
    return jnp.sum(jnp.where(at == to, jnp.broadcast_to(row, (size, size)), 0.0), axis=1, keepdims=True)


def columns_of(row):
    return jnp.transpose(jnp.broadcast_to(row, (8, row.shape[1])))[:, 0:1]


def inv_rms(values):
    return lax.rsqrt(jnp.mean(values * values, axis=-1, keepdims=True) + norm_eps)


def dispatch(groups, capacity, width, load, out_ref, table_ref):
    routes = load(0)[...]
    logits = load(1)[...]
    rows_b = routes.shape[1]
    expert = lax.broadcasted_iota(jnp.int32, (groups, rows_b), 0)
    first = expert == routes[0:1, :]
    second = expert == routes[1:2, :]
    named = jnp.where(first | second, 1.0, 0.0)
    before = lax.broadcasted_iota(jnp.int32, (rows_b, rows_b), 0) < lax.broadcasted_iota(jnp.int32, (rows_b, rows_b), 1)
    earlier = jnp.dot(named.astype(BF16), jnp.where(before, 1.0, 0.0).astype(BF16), preferred_element_type=F32)
    slot = expert.astype(F32) * capacity + earlier
    slot_a = jnp.sum(jnp.where(first, slot, 0.0), axis=0, keepdims=True)
    slot_b = jnp.sum(jnp.where(second, slot, 0.0), axis=0, keepdims=True)
    gap = logits[0:1, :] - logits[1:2, :]
    table_ref[...] = jnp.concatenate([slot_a, slot_b, jax.nn.sigmoid(gap), jax.nn.sigmoid(-gap), jnp.zeros((4, rows_b), F32)], axis=0)
    code = jnp.where(first | second, earlier, -1.0)
    place = lax.broadcasted_iota(jnp.int32, (groups, capacity, rows_b), 1).astype(F32)
    chosen = jnp.where(code[:, None, :] == place, 1.0, 0.0).reshape(groups * capacity, rows_b).astype(BF16)
    gain_ref, rows_ref = load(2), load(3)
    scale = inv_rms(rows_ref[...].astype(F32))
    start = pl.multiple_of(lax.axis_index("tp") * width, width)
    share = rows_ref[:, pl.ds(start, width)].astype(F32)
    normed = (share * scale * gain_ref[:, pl.ds(start, width)]).astype(BF16)
    out_ref[...] = jnp.dot(chosen, normed, preferred_element_type=F32).astype(BF16)


def mixer_front(load, gated_ref, taps_ref):
    taps_ref[...] = jnp.concatenate([load(0)[...], column_of(load(1)[...])], axis=1)
    gain_ref = load(2)
    rows = load(3)[...].astype(F32)
    normed = (rows * inv_rms(rows) * gain_ref[...]).astype(BF16)
    nt = (((1,), (1,)), ((), ()))
    value = lax.dot_general(load(4)[...], normed, nt, preferred_element_type=F32)
    gate = lax.dot_general(load(5)[...], normed, nt, preferred_element_type=F32)
    gated_ref[...] = (value * jax.nn.sigmoid(gate)).astype(BF16)


def conv_and_copies(arrived_ref, prev_ref, gated_ref, taps_ref, out_ref):
    count, _, width = out_ref.shape
    slots = arrived_ref.shape[0]
    taps = taps_ref[...]
    reach = taps.shape[1] - 2
    both = jnp.concatenate([prev_ref[...].astype(F32), gated_ref[...].astype(F32)], axis=1)
    span = both.shape[1]
    total = taps[:, reach + 1 :] + taps[:, reach : reach + 1] * both[:, width:]
    for k in range(reach):
        moved = pltpu.roll(both, reach - k, 1)
        total = total + taps[:, k : k + 1] * moved[:, span - width :]
    conv_out = total.astype(BF16)
    arrived = arrived_ref[...]
    for j in range(count):
        out_ref[j, :slots, :] = arrived
        out_ref[j, slots:, :] = conv_out


def swapped(j, side, swap):
    return jnp.where(swap, (j % side) * side + j // side, j)


def experts_and_mixer(slots, block, side, x_ref, wg_ref, wu_ref, wd_ref, cgain_ref, cshift_ref, wo_ref, out_ref, mix_ref):
    count, _, width = x_ref.shape
    odd = lax.axis_index("ep") % 2 == 1
    came = [swapped(j, side, odd) for j in range(count)]
    goes = [swapped(j, side, ~odd) for j in range(count)]
    wg, wu, wd = wg_ref[0], wu_ref[0], wd_ref[0]
    for at in range(0, slots, block):
        rows = jnp.concatenate([x_ref[came[j], at : at + block, :] for j in range(count)], axis=1)
        gate = jnp.dot(rows, wg, preferred_element_type=F32)
        up = jnp.dot(rows, wu, preferred_element_type=F32)
        hidden = (gate * jax.nn.sigmoid(gate) * up).astype(BF16)
        part = jnp.dot(hidden, wd, preferred_element_type=F32).astype(BF16)
        for j in range(count):
            out_ref[goes[j], at : at + block, :] = part[:, j * width : (j + 1) * width]
    values = jnp.concatenate([x_ref[came[j], slots:, :] for j in range(count)], axis=0).astype(F32)
    centered = values - jnp.mean(values, axis=0, keepdims=True)
    variance = jnp.mean(centered * centered, axis=0, keepdims=True)
    shaped = centered * lax.rsqrt(variance + norm_eps) * columns_of(cgain_ref[...]) + columns_of(cshift_ref[...])
    activated = (shaped * jax.nn.sigmoid(shaped)).astype(BF16)
    mix_ref[...] = lax.dot_general(activated, wo_ref[...], (((0,), (0,)), ((), ())), preferred_element_type=F32).astype(BF16)


def add_parts(parts_ref, out_ref):
    total = parts_ref[0].astype(F32)
    for j in range(1, parts_ref.shape[0]):
        total = total + parts_ref[j].astype(F32)
    out_ref[...] = total.astype(BF16)


def combine(back_ref, table_ref, out_ref):
    rows_b = out_ref.shape[0]
    slots = back_ref.shape[0]
    table = jnp.transpose(table_ref[...])
    place = lax.broadcasted_iota(jnp.int32, (rows_b, slots), 1).astype(F32)
    back = back_ref[...]
    total = None
    for j in range(2):
        pick = jnp.where(table[:, j : j + 1] == place, 1.0, 0.0).astype(BF16)
        term = jnp.dot(pick, back, preferred_element_type=F32) * table[:, 2 + j : 3 + j]
        total = term if total is None else total + term
    out_ref[...] = total.astype(BF16)


def exchange(blocks, axis, members=None):
    return lax.all_to_all(blocks, axis, split_axis=0, concat_axis=0, tiled=True, axis_index_groups=members)


def plane_groups(groups, side, first):
    members = []
    for e in range(groups):
        along_x = (e % 2 == 0) == first
        for a in range(side):
            members.append([e * side * side + (a * side + b if along_x else b * side + a) for b in range(side)])
    return members


def on_device(
    mixer_input,
    mixer_gain,
    glu_value_weight,
    glu_gate_weight,
    conv_taps,
    conv_bias,
    channel_gain,
    channel_shift,
    mixer_out_weight,
    expert_input,
    expert_gain,
    routes,
    route_logits,
    gate_weight,
    up_weight,
    down_weight,
):
    groups = lax.axis_size("ep")
    parts = lax.axis_size("tp")
    rows_b, features = expert_input.shape
    width = features // parts
    capacity = 3 * rows_b // groups
    slots = groups * capacity
    channels, tokens = glu_value_weight.shape[0], mixer_input.shape[0]

    side = math.isqrt(parts)
    plane = ("ep", "tp")
    line_one, line_two = plane_groups(groups, side, True), plane_groups(groups, side, False)

    def front(*refs):
        dispatch(groups, capacity, width, *refs)

    outgoing, table = staged(
        front,
        [((slots, width), BF16), ((8, rows_b), F32)],
        routes.T,
        route_logits.T,
        expert_gain[None, :],
        expert_input,
    )
    gated, taps = staged(
        mixer_front,
        [((channels, tokens), BF16), ((channels, conv_taps.shape[1] + 1), F32)],
        conv_taps,
        conv_bias[None, :],
        mixer_gain[None, :],
        mixer_input,
        glu_value_weight,
        glu_gate_weight,
    )
    before = lax.ppermute(gated, "ep", [(i, i + 1) for i in range(groups - 1)])
    arrived = exchange(outgoing.reshape(groups, capacity, width), "ep").reshape(slots, width)
    held = slots + channels
    (copies,) = call(conv_and_copies, [((side, held, width), BF16)], arrived, before, gated, taps)
    line = exchange(copies, plane, line_one).reshape(side * held, width)
    gathered = exchange(jnp.broadcast_to(line, (side, *line.shape)), plane, line_two)

    def middle(*refs):
        experts_and_mixer(slots, 256, side, *refs)

    partial, mixed = call(
        middle,
        [((parts, slots, width), BF16), ((tokens, width), BF16)],
        gathered.reshape(parts, held, width),
        gate_weight,
        up_weight,
        down_weight,
        channel_gain[None, :],
        channel_shift[None, :],
        mixer_out_weight,
    )
    (line_sum,) = call(add_parts, [((side * slots, width), BF16)], exchange(partial.reshape(side, side * slots, width), plane, line_one))
    (summed,) = call(add_parts, [((slots, width), BF16)], exchange(line_sum.reshape(side, slots, width), plane, line_two))
    returned = exchange(summed.reshape(groups, capacity, width), "ep").reshape(slots, width)
    (combined,) = call(combine, [((rows_b, width), BF16)], returned, table)
    return mixed, combined


def solution(mesh):
    in_specs = (
        P("ep", None),
        P(),
        P("tp", None),
        P("tp", None),
        P("tp", None),
        P("tp"),
        P(),
        P(),
        P(None, "tp"),
        P("ep", None),
        P(),
        P("ep", None),
        P("ep", None),
        P("ep", None, "tp"),
        P("ep", None, "tp"),
        P("ep", "tp", None),
    )
    out_specs = (P("ep", "tp"), P("ep", "tp"))
    return jax.shard_map(
        on_device, mesh=mesh, in_specs=in_specs, out_specs=out_specs, check_vma=False
    )
```

```python
import math

import jax
import jax.numpy as jnp
from jax import lax
from jax.experimental import pallas as pl
from jax.experimental.pallas import tpu as pltpu
from jax.sharding import PartitionSpec as P

norm_eps = 1e-06
F32 = jnp.float32
BF16 = jnp.bfloat16


def whole(space, count):
    return [pl.BlockSpec(memory_space=space)] * count


def call(body, outs, *operands, source=pltpu.VMEM, scratch=()):
    return pl.pallas_call(
        body,
        out_shape=tuple(jax.ShapeDtypeStruct(s, d) for s, d in outs),
        in_specs=whole(source, len(operands)),
        out_specs=tuple(whole(pltpu.VMEM, len(outs))),
        scratch_shapes=list(scratch),
        compiler_params=pltpu.CompilerParams(vmem_limit_bytes=20 * 1024 * 1024),
    )(*operands)


def staged(body, outs, *operands):
    count = len(operands)

    def kernel(*refs):
        sources, results = refs[:count], refs[count : count + len(outs)]
        held, sems = refs[count + len(outs) : -1], refs[-1]
        copies = [pltpu.make_async_copy(sources[i], held[i], sems.at[i]) for i in range(count)]
        for copy in copies:
            copy.start()

        def load(i):
            copies[i].wait()
            return held[i]

        body(load, *results)

    scratch = [pltpu.VMEM(x.shape, x.dtype) for x in operands] + [pltpu.SemaphoreType.DMA((count,))]
    pinned = [pltpu.with_memory_space_constraint(x, pltpu.HBM) for x in operands]
    return call(kernel, outs, *pinned, source=pltpu.HBM, scratch=scratch)


def column_of(row):
    size = row.shape[1]
    at = lax.broadcasted_iota(jnp.int32, (size, size), 0)
    to = lax.broadcasted_iota(jnp.int32, (size, size), 1)
    return jnp.sum(jnp.where(at == to, jnp.broadcast_to(row, (size, size)), 0.0), axis=1, keepdims=True)


def columns_of(row):
    return jnp.transpose(jnp.broadcast_to(row, (8, row.shape[1])))[:, 0:1]


def inv_rms(values):
    return lax.rsqrt(jnp.mean(values * values, axis=-1, keepdims=True) + norm_eps)


def dispatch(groups, capacity, width, load, out_ref, table_ref):
    routes = load(0)[...]
    logits = load(1)[...]
    rows_b = routes.shape[1]
    expert = lax.broadcasted_iota(jnp.int32, (groups, rows_b), 0)
    first = expert == routes[0:1, :]
    second = expert == routes[1:2, :]
    named = jnp.where(first | second, 1.0, 0.0)
    before = lax.broadcasted_iota(jnp.int32, (rows_b, rows_b), 0) < lax.broadcasted_iota(jnp.int32, (rows_b, rows_b), 1)
    earlier = jnp.dot(named.astype(BF16), jnp.where(before, 1.0, 0.0).astype(BF16), preferred_element_type=F32)
    slot = expert.astype(F32) * capacity + earlier
    slot_a = jnp.sum(jnp.where(first, slot, 0.0), axis=0, keepdims=True)
    slot_b = jnp.sum(jnp.where(second, slot, 0.0), axis=0, keepdims=True)
    gap = logits[0:1, :] - logits[1:2, :]
    table_ref[...] = jnp.concatenate([slot_a, slot_b, jax.nn.sigmoid(gap), jax.nn.sigmoid(-gap), jnp.zeros((4, rows_b), F32)], axis=0)
    code = jnp.where(first | second, earlier, -1.0)
    place = lax.broadcasted_iota(jnp.int32, (groups, capacity, rows_b), 1).astype(F32)
    chosen = jnp.where(code[:, None, :] == place, 1.0, 0.0).reshape(groups * capacity, rows_b).astype(BF16)
    gain_ref, rows_ref = load(2), load(3)
    scale = inv_rms(rows_ref[...].astype(F32))
    start = pl.multiple_of(lax.axis_index("tp") * width, width)
    share = rows_ref[:, pl.ds(start, width)].astype(F32)
    normed = (share * scale * gain_ref[:, pl.ds(start, width)]).astype(BF16)
    out_ref[...] = jnp.dot(chosen, normed, preferred_element_type=F32).astype(BF16)


def mixer_front(load, gated_ref, taps_ref):
    taps_ref[...] = jnp.concatenate([load(0)[...], column_of(load(1)[...])], axis=1)
    gain_ref = load(2)
    rows = load(3)[...].astype(F32)
    normed = (rows * inv_rms(rows) * gain_ref[...]).astype(BF16)
    nt = (((1,), (1,)), ((), ()))
    value = lax.dot_general(load(4)[...], normed, nt, preferred_element_type=F32)
    gate = lax.dot_general(load(5)[...], normed, nt, preferred_element_type=F32)
    gated_ref[...] = (value * jax.nn.sigmoid(gate)).astype(BF16)


def conv_and_copies(arrived_ref, prev_ref, gated_ref, taps_ref, out_ref):
    count, _, width = out_ref.shape
    slots = arrived_ref.shape[0]
    taps = taps_ref[...]
    reach = taps.shape[1] - 2
    both = jnp.concatenate([prev_ref[...].astype(F32), gated_ref[...].astype(F32)], axis=1)
    span = both.shape[1]
    total = taps[:, reach + 1 :] + taps[:, reach : reach + 1] * both[:, width:]
    for k in range(reach):
        moved = pltpu.roll(both, reach - k, 1)
        total = total + taps[:, k : k + 1] * moved[:, span - width :]
    conv_out = total.astype(BF16)
    arrived = arrived_ref[...]
    for j in range(count):
        out_ref[j, :slots, :] = arrived
        out_ref[j, slots:, :] = conv_out


def plane_places(side):
    odd = lax.axis_index("ep") % 2
    here = lax.axis_index("tp")

    def steps(at):
        base = (at - odd + side) % side // 2 * 2
        return [(k + 1 - odd - base + side) % side for k in range(side)]

    down, across = steps(here // side), steps(here % side)
    return [
        ((down[j // side] // 2) * 2 + across[j % side] // 2) * 4 + (down[j // side] % 2) * 2 + across[j % side] % 2
        for j in range(side * side)
    ]


def experts_and_mixer(slots, block, side, x_ref, wg_ref, wu_ref, wd_ref, cgain_ref, cshift_ref, wo_ref, out_ref, mix_ref):
    count, _, width = x_ref.shape
    place = plane_places(side)
    wg, wu, wd = wg_ref[0], wu_ref[0], wd_ref[0]
    for at in range(0, slots, block):
        rows = jnp.concatenate([x_ref[place[j], at : at + block, :] for j in range(count)], axis=1)
        gate = jnp.dot(rows, wg, preferred_element_type=F32)
        up = jnp.dot(rows, wu, preferred_element_type=F32)
        hidden = (gate * jax.nn.sigmoid(gate) * up).astype(BF16)
        part = jnp.dot(hidden, wd, preferred_element_type=F32).astype(BF16)
        for j in range(count):
            out_ref[place[j], at : at + block, :] = part[:, j * width : (j + 1) * width]
    values = jnp.concatenate([x_ref[place[j], slots:, :] for j in range(count)], axis=0).astype(F32)
    centered = values - jnp.mean(values, axis=0, keepdims=True)
    variance = jnp.mean(centered * centered, axis=0, keepdims=True)
    shaped = centered * lax.rsqrt(variance + norm_eps) * columns_of(cgain_ref[...]) + columns_of(cshift_ref[...])
    activated = (shaped * jax.nn.sigmoid(shaped)).astype(BF16)
    mix_ref[...] = lax.dot_general(activated, wo_ref[...], (((0,), (0,)), ((), ())), preferred_element_type=F32).astype(BF16)


def add_parts(parts_ref, out_ref):
    total = parts_ref[0].astype(F32)
    for j in range(1, parts_ref.shape[0]):
        total = total + parts_ref[j].astype(F32)
    out_ref[...] = total.astype(BF16)


def combine(back_ref, table_ref, out_ref):
    rows_b = out_ref.shape[0]
    slots = back_ref.shape[0]
    table = jnp.transpose(table_ref[...])
    place = lax.broadcasted_iota(jnp.int32, (rows_b, slots), 1).astype(F32)
    back = back_ref[...]
    total = None
    for j in range(2):
        pick = jnp.where(table[:, j : j + 1] == place, 1.0, 0.0).astype(BF16)
        term = jnp.dot(pick, back, preferred_element_type=F32) * table[:, 2 + j : 3 + j]
        total = term if total is None else total + term
    out_ref[...] = total.astype(BF16)


def exchange(blocks, axis, members=None):
    return lax.all_to_all(blocks, axis, split_axis=0, concat_axis=0, tiled=True, axis_index_groups=members)


def plane_groups(groups, side, turned):
    half = side // 2
    members = []
    for e in range(groups):
        shift = (e + turned) % 2
        for by in range(half):
            for bx in range(half):
                members.append([
                    e * side * side + (2 * by + oy + shift) % side * side + (2 * bx + ox + shift) % side
                    for oy in range(2)
                    for ox in range(2)
                ])
    return members


def on_device(
    mixer_input,
    mixer_gain,
    glu_value_weight,
    glu_gate_weight,
    conv_taps,
    conv_bias,
    channel_gain,
    channel_shift,
    mixer_out_weight,
    expert_input,
    expert_gain,
    routes,
    route_logits,
    gate_weight,
    up_weight,
    down_weight,
):
    groups = lax.axis_size("ep")
    parts = lax.axis_size("tp")
    rows_b, features = expert_input.shape
    width = features // parts
    capacity = 3 * rows_b // groups
    slots = groups * capacity
    channels, tokens = glu_value_weight.shape[0], mixer_input.shape[0]

    side = math.isqrt(parts)
    plane = ("ep", "tp")
    inner, outer = plane_groups(groups, side, 1), plane_groups(groups, side, 0)

    def front(*refs):
        dispatch(groups, capacity, width, *refs)

    outgoing, table = staged(
        front,
        [((slots, width), BF16), ((8, rows_b), F32)],
        routes.T,
        route_logits.T,
        expert_gain[None, :],
        expert_input,
    )
    gated, taps = staged(
        mixer_front,
        [((channels, tokens), BF16), ((channels, conv_taps.shape[1] + 1), F32)],
        conv_taps,
        conv_bias[None, :],
        mixer_gain[None, :],
        mixer_input,
        glu_value_weight,
        glu_gate_weight,
    )
    before = lax.ppermute(gated, "ep", [(i, i + 1) for i in range(groups - 1)])
    arrived = exchange(outgoing.reshape(groups, capacity, width), "ep").reshape(slots, width)
    held = slots + channels
    (copies,) = call(conv_and_copies, [((side, held, width), BF16)], arrived, before, gated, taps)
    block = exchange(copies, plane, inner).reshape(side * held, width)
    gathered = exchange(jnp.broadcast_to(block, (side, *block.shape)), plane, outer)

    def middle(*refs):
        experts_and_mixer(slots, 256, side, *refs)

    partial, mixed = call(
        middle,
        [((parts, slots, width), BF16), ((tokens, width), BF16)],
        gathered.reshape(parts, held, width),
        gate_weight,
        up_weight,
        down_weight,
        channel_gain[None, :],
        channel_shift[None, :],
        mixer_out_weight,
    )
    (block_sum,) = call(add_parts, [((side * slots, width), BF16)], exchange(partial.reshape(side, side * slots, width), plane, outer))
    (summed,) = call(add_parts, [((slots, width), BF16)], exchange(block_sum.reshape(side, slots, width), plane, inner))
    returned = exchange(summed.reshape(groups, capacity, width), "ep").reshape(slots, width)
    (combined,) = call(combine, [((rows_b, width), BF16)], returned, table)
    return mixed, combined


def solution(mesh):
    in_specs = (
        P("ep", None),
        P(),
        P("tp", None),
        P("tp", None),
        P("tp", None),
        P("tp"),
        P(),
        P(),
        P(None, "tp"),
        P("ep", None),
        P(),
        P("ep", None),
        P("ep", None),
        P("ep", None, "tp"),
        P("ep", None, "tp"),
        P("ep", "tp", None),
    )
    out_specs = (P("ep", "tp"), P("ep", "tp"))
    return jax.shard_map(
        on_device, mesh=mesh, in_specs=in_specs, out_specs=out_specs, check_vma=False
    )
```

```python
import math

import jax
import jax.numpy as jnp
from jax import lax
from jax.experimental import pallas as pl
from jax.experimental.pallas import tpu as pltpu
from jax.sharding import PartitionSpec as P


norm_eps = 1e-06
F32 = jnp.float32
BF16 = jnp.bfloat16


def call(body, outs, *operands, far=0):
    near = len(operands) - far
    operands = operands[:near] + tuple(pltpu.with_memory_space_constraint(x, pltpu.HBM) for x in operands[near:])

    def kernel(*refs):
        sources, results = refs[near : near + far], refs[near + far : near + far + len(outs)]
        if not far:
            body(*refs[:near], *results)
            return
        held, sems = refs[near + far + len(outs) : -1], refs[-1]
        copies = [pltpu.make_async_copy(sources[i], held[i], sems.at[i]) for i in range(far)]
        for copy in copies:
            copy.start()
        ready = set()

        def load(i):
            if i not in ready:
                copies[i].wait()
                ready.add(i)
            return held[i]

        body(load, *refs[:near], *results)

    scratch = [pltpu.VMEM(x.shape, x.dtype) for x in operands[near:]]
    return pl.pallas_call(
        kernel,
        out_shape=tuple(jax.ShapeDtypeStruct(s, d) for s, d in outs),
        in_specs=[pl.BlockSpec(memory_space=pltpu.VMEM)] * near + [pl.BlockSpec(memory_space=pltpu.HBM)] * far,
        out_specs=tuple([pl.BlockSpec(memory_space=pltpu.VMEM)] * len(outs)),
        scratch_shapes=scratch + [pltpu.SemaphoreType.DMA((far,))] * (far > 0),
        compiler_params=pltpu.CompilerParams(vmem_limit_bytes=20 * 1024 * 1024),
    )(*operands)


def column_of(row):
    size = row.shape[1]
    at = lax.broadcasted_iota(jnp.int32, (size, size), 0)
    to = lax.broadcasted_iota(jnp.int32, (size, size), 1)
    return jnp.sum(jnp.where(at == to, jnp.broadcast_to(row, (size, size)), 0.0), axis=1, keepdims=True)


def columns_of(row):
    return jnp.transpose(jnp.broadcast_to(row, (8, row.shape[1])))[:, 0:1]


def inv_rms(values):
    return lax.rsqrt(jnp.mean(values * values, axis=-1, keepdims=True) + norm_eps)


def dispatch(groups, capacity, width, load, out_ref, table_ref):
    routes = load(0)[...]
    logits = load(1)[...]
    rows_b = routes.shape[1]
    expert = lax.broadcasted_iota(jnp.int32, (groups, rows_b), 0)
    first = expert == routes[0:1, :]
    second = expert == routes[1:2, :]
    named = jnp.where(first | second, 1.0, 0.0)
    before = lax.broadcasted_iota(jnp.int32, (rows_b, rows_b), 0) < lax.broadcasted_iota(jnp.int32, (rows_b, rows_b), 1)
    earlier = jnp.dot(named.astype(BF16), jnp.where(before, 1.0, 0.0).astype(BF16), preferred_element_type=F32)
    slot = expert.astype(F32) * capacity + earlier
    slot_a = jnp.sum(jnp.where(first, slot, 0.0), axis=0, keepdims=True)
    slot_b = jnp.sum(jnp.where(second, slot, 0.0), axis=0, keepdims=True)
    gap = logits[0:1, :] - logits[1:2, :]
    table_ref[...] = jnp.concatenate([slot_a, slot_b, jax.nn.sigmoid(gap), jax.nn.sigmoid(-gap), jnp.zeros((4, rows_b), F32)], axis=0)
    code = jnp.where(first | second, earlier, -1.0)
    place = lax.broadcasted_iota(jnp.int32, (groups, capacity, rows_b), 1).astype(F32)
    chosen = jnp.where(code[:, None, :] == place, 1.0, 0.0).reshape(groups * capacity, rows_b).astype(BF16)
    gain_ref, rows_ref = load(2), load(3)
    scale = inv_rms(rows_ref[...].astype(F32))
    start = pl.multiple_of(lax.axis_index("tp") * width, width)
    share = rows_ref[:, pl.ds(start, width)].astype(F32)
    normed = (share * scale * gain_ref[:, pl.ds(start, width)]).astype(BF16)
    out_ref[...] = jnp.dot(chosen, normed, preferred_element_type=F32).astype(BF16)


def mixer_front(load, gated_ref, taps_ref):
    taps_ref[...] = jnp.concatenate([load(0)[...], column_of(load(1)[...])], axis=1)
    gain_ref = load(2)
    rows = load(3)[...].astype(F32)
    normed = (rows * inv_rms(rows) * gain_ref[...]).astype(BF16)
    nt = (((1,), (1,)), ((), ()))
    value = lax.dot_general(load(4)[...], normed, nt, preferred_element_type=F32)
    gate = lax.dot_general(load(5)[...], normed, nt, preferred_element_type=F32)
    gated_ref[...] = (value * jax.nn.sigmoid(gate)).astype(BF16)


def conv_and_copies(side, arrived_ref, prev_ref, gated_ref, taps_ref, out_ref):
    count, _, width = out_ref.shape
    half = arrived_ref.shape[0] // 2
    taps = taps_ref[...]
    reach = taps.shape[1] - 2
    both = jnp.concatenate([prev_ref[...].astype(F32), gated_ref[...].astype(F32)], axis=1)
    span = both.shape[1]
    total = taps[:, reach + 1 :] + taps[:, reach : reach + 1] * both[:, width:]
    for k in range(reach):
        moved = pltpu.roll(both, reach - k, 1)
        total = total + taps[:, k : k + 1] * moved[:, span - width :]
    conv_out = total.astype(BF16)
    odd = lax.axis_index("ep") % 2
    for p in range(2):
        start = pl.multiple_of((p + odd) % 2 * half, half)
        rows = arrived_ref[pl.ds(start, half), :]
        for j in range(count):
            if j % side % 2 == p:
                out_ref[j, :half, :] = rows
                out_ref[j, half:, :] = conv_out


def shard_part(rows, gate_ref, up_ref, down_ref):
    gate = jnp.dot(rows, gate_ref[0], preferred_element_type=F32)
    up = jnp.dot(rows, up_ref[0], preferred_element_type=F32)
    hidden = (gate * jax.nn.sigmoid(gate) * up).astype(BF16)
    return jnp.dot(hidden, down_ref[0], preferred_element_type=F32)


def own_shard(slots, x_ref, wg_ref, wu_ref, wd_ref, cgain_ref, cshift_ref, wo_ref, part_ref, mix_ref):
    count = x_ref.shape[0]
    rows = jnp.concatenate([x_ref[j, :slots, :] for j in range(count)], axis=1)
    part_ref[...] = shard_part(rows, wg_ref, wu_ref, wd_ref)
    values = jnp.concatenate([x_ref[j, slots:, :] for j in range(count)], axis=0).astype(F32)
    centered = values - jnp.mean(values, axis=0, keepdims=True)
    variance = jnp.mean(centered * centered, axis=0, keepdims=True)
    shaped = centered * lax.rsqrt(variance + norm_eps) * columns_of(cgain_ref[...]) + columns_of(cshift_ref[...])
    activated = (shaped * jax.nn.sigmoid(shaped)).astype(BF16)
    mix_ref[...] = lax.dot_general(activated, wo_ref[...], (((0,), (0,)), ((), ())), preferred_element_type=F32).astype(BF16)


def lent_shard(x_ref, part_ref, wg_ref, wu_ref, wd_ref, out_ref):
    count, slots, width = out_ref.shape
    rows = jnp.concatenate([x_ref[j, :slots, :] for j in range(count)], axis=1)
    total = (part_ref[...] + shard_part(rows, wg_ref, wu_ref, wd_ref)).astype(BF16)
    for j in range(count):
        out_ref[j] = total[:, j * width : (j + 1) * width]


def add_parts(side, parts_ref, out_ref):
    count, half, _ = parts_ref.shape
    odd = lax.axis_index("ep") % 2
    for p in range(2):
        total = None
        for j in range(count):
            if j % side % 2 == p:
                term = parts_ref[j].astype(F32)
                total = term if total is None else total + term
        start = pl.multiple_of((p + odd) % 2 * half, half)
        out_ref[pl.ds(start, half), :] = total.astype(BF16)


def combine(back_ref, table_ref, out_ref):
    rows_b = out_ref.shape[0]
    slots = back_ref.shape[0]
    table = jnp.transpose(table_ref[...])
    place = lax.broadcasted_iota(jnp.int32, (rows_b, slots), 1).astype(F32)
    back = back_ref[...]
    total = None
    for j in range(2):
        pick = jnp.where(table[:, j : j + 1] == place, 1.0, 0.0).astype(BF16)
        term = jnp.dot(pick, back, preferred_element_type=F32) * table[:, 2 + j : 3 + j]
        total = term if total is None else total + term
    out_ref[...] = total.astype(BF16)


def exchange(blocks, axis):
    return lax.all_to_all(blocks, axis, split_axis=0, concat_axis=0, tiled=True)


def neighbours(groups, side):
    pairs = []
    for e in range(groups):
        shift = e % 2
        for y in range(side):
            for x in range(side):
                pairs.append(((e * side + y) * side + x, (e * side + y) * side + (((x - shift) % side ^ 1) + shift) % side))
    return pairs


def on_device(
    mixer_input,
    mixer_gain,
    glu_value_weight,
    glu_gate_weight,
    conv_taps,
    conv_bias,
    channel_gain,
    channel_shift,
    mixer_out_weight,
    expert_input,
    expert_gain,
    routes,
    route_logits,
    gate_weight,
    up_weight,
    down_weight,
):
    groups = lax.axis_size("ep")
    parts = lax.axis_size("tp")
    rows_b, features = expert_input.shape
    width = features // parts
    capacity = 3 * rows_b // groups
    slots = groups * capacity
    channels, tokens = glu_value_weight.shape[0], mixer_input.shape[0]

    side = math.isqrt(parts)
    half = slots // 2
    pairs = neighbours(groups, side)
    shards = (gate_weight, up_weight, down_weight)
    lent = []
    for w in shards:
        lent.append(lax.ppermute(w, ("ep", "tp"), pairs))

    def front(*refs):
        dispatch(groups, capacity, width, *refs)

    outgoing, table = call(
        front,
        [((slots, width), BF16), ((8, rows_b), F32)],
        routes.T,
        route_logits.T,
        expert_gain[None, :],
        expert_input,
        far=4,
    )
    gated, taps = call(
        mixer_front,
        [((channels, tokens), BF16), ((channels, conv_taps.shape[1] + 1), F32)],
        conv_taps,
        conv_bias[None, :],
        mixer_gain[None, :],
        mixer_input,
        glu_value_weight,
        glu_gate_weight,
        far=6,
    )
    before = lax.ppermute(gated, "ep", [(i, i + 1) for i in range(groups - 1)])
    arrived = exchange(outgoing.reshape(groups, capacity, width), "ep").reshape(slots, width)

    def spread(*refs):
        conv_and_copies(side, *refs)

    (copies,) = call(spread, [((parts, half + channels, width), BF16)], arrived, before, gated, taps)
    gathered = exchange(copies, "tp")

    def own(*refs):
        own_shard(half, *refs)

    part, mixed = call(
        own,
        [((half, features), F32), ((tokens, width), BF16)],
        gathered,
        *shards,
        channel_gain[None, :],
        channel_shift[None, :],
        mixer_out_weight,
    )
    (partial,) = call(lent_shard, [((parts, half, width), BF16)], gathered, part, *lent)

    def total(*refs):
        add_parts(side, *refs)

    (summed,) = call(total, [((slots, width), BF16)], exchange(partial, "tp"))
    returned = exchange(summed.reshape(groups, capacity, width), "ep").reshape(slots, width)
    (combined,) = call(combine, [((rows_b, width), BF16)], returned, table)
    return mixed, combined


def solution(mesh):
    in_specs = (
        P("ep", None),
        P(),
        P("tp", None),
        P("tp", None),
        P("tp", None),
        P("tp"),
        P(),
        P(),
        P(None, "tp"),
        P("ep", None),
        P(),
        P("ep", None),
        P("ep", None),
        P("ep", None, "tp"),
        P("ep", None, "tp"),
        P("ep", "tp", None),
    )
    out_specs = (P("ep", "tp"), P("ep", "tp"))

    return jax.shard_map(on_device, mesh=mesh, in_specs=in_specs, out_specs=out_specs, check_vma=False)
```

```python
import math

import jax
import jax.numpy as jnp
from jax import lax
from jax.experimental import pallas as pl
from jax.experimental.pallas import tpu as pltpu
from jax.sharding import PartitionSpec as P


norm_eps = 1e-06
F32 = jnp.float32
BF16 = jnp.bfloat16


def call(body, outs, *operands, far=0):
    near = len(operands) - far
    operands = operands[:near] + tuple(pltpu.with_memory_space_constraint(x, pltpu.HBM) for x in operands[near:])

    def kernel(*refs):
        sources, results = refs[near : near + far], refs[near + far : near + far + len(outs)]
        if not far:
            body(*refs[:near], *results)
            return
        held, sems = refs[near + far + len(outs) : -1], refs[-1]
        copies = [pltpu.make_async_copy(sources[i], held[i], sems.at[i]) for i in range(far)]
        for copy in copies:
            copy.start()
        ready = set()

        def load(i):
            if i not in ready:
                copies[i].wait()
                ready.add(i)
            return held[i]

        body(load, *refs[:near], *results)

    scratch = [pltpu.VMEM(x.shape, x.dtype) for x in operands[near:]]
    return pl.pallas_call(
        kernel,
        out_shape=tuple(jax.ShapeDtypeStruct(s, d) for s, d in outs),
        in_specs=[pl.BlockSpec(memory_space=pltpu.VMEM)] * near + [pl.BlockSpec(memory_space=pltpu.HBM)] * far,
        out_specs=tuple([pl.BlockSpec(memory_space=pltpu.VMEM)] * len(outs)),
        scratch_shapes=scratch + [pltpu.SemaphoreType.DMA((far,))] * (far > 0),
        compiler_params=pltpu.CompilerParams(vmem_limit_bytes=20 * 1024 * 1024),
    )(*operands)


def column_of(row):
    size = row.shape[1]
    at = lax.broadcasted_iota(jnp.int32, (size, size), 0)
    to = lax.broadcasted_iota(jnp.int32, (size, size), 1)
    return jnp.sum(jnp.where(at == to, jnp.broadcast_to(row, (size, size)), 0.0), axis=1, keepdims=True)


def columns_of(row):
    return jnp.transpose(jnp.broadcast_to(row, (8, row.shape[1])))[:, 0:1]


def inv_rms(values):
    return lax.rsqrt(jnp.mean(values * values, axis=-1, keepdims=True) + norm_eps)


def dispatch(groups, capacity, width, load, out_ref, table_ref):
    routes = load(0)[...]
    logits = load(1)[...]
    rows_b = routes.shape[1]
    expert = lax.broadcasted_iota(jnp.int32, (groups, rows_b), 0)
    first = expert == routes[0:1, :]
    second = expert == routes[1:2, :]
    named = jnp.where(first | second, 1.0, 0.0)
    before = lax.broadcasted_iota(jnp.int32, (rows_b, rows_b), 0) < lax.broadcasted_iota(jnp.int32, (rows_b, rows_b), 1)
    earlier = jnp.dot(named.astype(BF16), jnp.where(before, 1.0, 0.0).astype(BF16), preferred_element_type=F32)
    slot = expert.astype(F32) * capacity + earlier
    slot_a = jnp.sum(jnp.where(first, slot, 0.0), axis=0, keepdims=True)
    slot_b = jnp.sum(jnp.where(second, slot, 0.0), axis=0, keepdims=True)
    gap = logits[0:1, :] - logits[1:2, :]
    table_ref[...] = jnp.concatenate([slot_a, slot_b, jax.nn.sigmoid(gap), jax.nn.sigmoid(-gap), jnp.zeros((4, rows_b), F32)], axis=0)
    code = jnp.where(first | second, earlier, -1.0)
    place = lax.broadcasted_iota(jnp.int32, (groups, capacity, rows_b), 1).astype(F32)
    chosen = jnp.where(code[:, None, :] == place, 1.0, 0.0).reshape(groups * capacity, rows_b).astype(BF16)
    gain_ref, rows_ref = load(2), load(3)
    scale = inv_rms(rows_ref[...].astype(F32))
    start = pl.multiple_of(lax.axis_index("tp") * width, width)
    share = rows_ref[:, pl.ds(start, width)].astype(F32)
    normed = (share * scale * gain_ref[:, pl.ds(start, width)]).astype(BF16)
    out_ref[...] = jnp.dot(chosen, normed, preferred_element_type=F32).astype(BF16)


def mixer_front(load, gated_ref, taps_ref):
    taps_ref[...] = jnp.concatenate([load(0)[...], column_of(load(1)[...])], axis=1)
    gain_ref = load(2)
    rows = load(3)[...].astype(F32)
    normed = (rows * inv_rms(rows) * gain_ref[...]).astype(BF16)
    nt = (((1,), (1,)), ((), ()))
    value = lax.dot_general(load(4)[...], normed, nt, preferred_element_type=F32)
    gate = lax.dot_general(load(5)[...], normed, nt, preferred_element_type=F32)
    gated_ref[...] = (value * jax.nn.sigmoid(gate)).astype(BF16)


def row_class(j, side):
    return (j // side + j % side) % 2


def spread_rows(side, arrived_ref, out_ref):
    half = out_ref.shape[1]
    for j in range(out_ref.shape[0]):
        p = row_class(j, side)
        out_ref[j] = arrived_ref[p * half : (p + 1) * half, :]


def convolved(prev_ref, gated_ref, taps_ref):
    width = gated_ref.shape[1]
    taps = taps_ref[...]
    reach = taps.shape[1] - 2
    both = jnp.concatenate([prev_ref[...].astype(F32), gated_ref[...].astype(F32)], axis=1)
    span = both.shape[1]
    total = taps[:, reach + 1 :] + taps[:, reach : reach + 1] * both[:, width:]
    for k in range(reach):
        moved = pltpu.roll(both, reach - k, 1)
        total = total + taps[:, k : k + 1] * moved[:, span - width :]
    return total.astype(BF16)


def shard_part(rows, gate_ref, up_ref, down_ref):
    gate = jnp.dot(rows, gate_ref[0], preferred_element_type=F32)
    up = jnp.dot(rows, up_ref[0], preferred_element_type=F32)
    hidden = (gate * jax.nn.sigmoid(gate) * up).astype(BF16)
    return jnp.dot(hidden, down_ref[0], preferred_element_type=F32)


def own_shard(x_ref, wg_ref, wu_ref, wd_ref, part_ref):
    rows = jnp.concatenate([x_ref[j] for j in range(x_ref.shape[0])], axis=1)
    part_ref[...] = shard_part(rows, wg_ref, wu_ref, wd_ref)


def lent_shard(x_ref, part_ref, wg_ref, wu_ref, wd_ref, prev_ref, gated_ref, taps_ref, out_ref):
    count, slots, width = x_ref.shape
    conv_out = convolved(prev_ref, gated_ref, taps_ref)
    for j in range(count):
        out_ref[j, slots:, :] = conv_out
    rows = jnp.concatenate([x_ref[j] for j in range(count)], axis=1)
    total = (part_ref[...] + shard_part(rows, wg_ref, wu_ref, wd_ref)).astype(BF16)
    for j in range(count):
        out_ref[j, :slots, :] = total[:, j * width : (j + 1) * width]


def mixer_tail(slots, parts_ref, cgain_ref, cshift_ref, wo_ref, out_ref):
    values = jnp.concatenate([parts_ref[j, slots:, :] for j in range(parts_ref.shape[0])], axis=0).astype(F32)
    centered = values - jnp.mean(values, axis=0, keepdims=True)
    variance = jnp.mean(centered * centered, axis=0, keepdims=True)
    shaped = centered * lax.rsqrt(variance + norm_eps) * columns_of(cgain_ref[...]) + columns_of(cshift_ref[...])
    activated = (shaped * jax.nn.sigmoid(shaped)).astype(BF16)
    out_ref[...] = lax.dot_general(activated, wo_ref[...], (((0,), (0,)), ((), ())), preferred_element_type=F32).astype(BF16)


def add_parts(side, parts_ref, out_ref):
    count, half = parts_ref.shape[0], out_ref.shape[0] // 2
    for p in range(2):
        total = None
        for j in range(count):
            if row_class(j, side) == p:
                term = parts_ref[j, :half, :].astype(F32)
                total = term if total is None else total + term
        out_ref[p * half : (p + 1) * half, :] = total.astype(BF16)


def combine(back_ref, table_ref, out_ref):
    rows_b = out_ref.shape[0]
    slots = back_ref.shape[0]
    table = jnp.transpose(table_ref[...])
    place = lax.broadcasted_iota(jnp.int32, (rows_b, slots), 1).astype(F32)
    back = back_ref[...]
    total = None
    for j in range(2):
        pick = jnp.where(table[:, j : j + 1] == place, 1.0, 0.0).astype(BF16)
        term = jnp.dot(pick, back, preferred_element_type=F32) * table[:, 2 + j : 3 + j]
        total = term if total is None else total + term
    out_ref[...] = total.astype(BF16)


def exchange(blocks, axis):
    return lax.all_to_all(blocks, axis, split_axis=0, concat_axis=0, tiled=True)


def neighbours(groups, side, along_x):
    pairs = []
    for e in range(groups):
        shift = e % 2

        def other(at):
            return (((at - shift) % side ^ 1) + shift) % side

        for y in range(side):
            for x in range(side):
                to = (y, other(x)) if along_x else (other(y), x)
                pairs.append(((e * side + y) * side + x, (e * side + to[0]) * side + to[1]))
    return pairs


def on_device(
    mixer_input,
    mixer_gain,
    glu_value_weight,
    glu_gate_weight,
    conv_taps,
    conv_bias,
    channel_gain,
    channel_shift,
    mixer_out_weight,
    expert_input,
    expert_gain,
    routes,
    route_logits,
    gate_weight,
    up_weight,
    down_weight,
):
    groups = lax.axis_size("ep")
    parts = lax.axis_size("tp")
    rows_b, features = expert_input.shape
    width = features // parts
    capacity = 3 * rows_b // groups
    slots = groups * capacity
    channels, tokens = glu_value_weight.shape[0], mixer_input.shape[0]

    side = math.isqrt(parts)
    half = slots // 2
    shards = (gate_weight, up_weight, down_weight)


    def front(*refs):
        dispatch(groups, capacity, width, *refs)

    outgoing, table = call(
        front,
        [((slots, width), BF16), ((8, rows_b), F32)],
        routes.T,
        route_logits.T,
        expert_gain[None, :],
        expert_input,
        far=4,
    )
    gated, taps = call(
        mixer_front,
        [((channels, tokens), BF16), ((channels, conv_taps.shape[1] + 1), F32)],
        conv_taps,
        conv_bias[None, :],
        mixer_gain[None, :],
        mixer_input,
        glu_value_weight,
        glu_gate_weight,
        far=6,
    )
    before = lax.ppermute(gated, "ep", [(i, i + 1) for i in range(groups - 1)])
    lent = []
    for w in shards:
        lent.append(lax.ppermute(w, ("ep", "tp"), neighbours(groups, side, True)))
    arrived = exchange(outgoing.reshape(groups, capacity, width), "ep").reshape(slots, width)

    def spread(*refs):
        spread_rows(side, *refs)

    (copies,) = call(spread, [((parts, half, width), BF16)], arrived)
    gathered = exchange(copies, "tp")
    (part,) = call(own_shard, [((half, features), F32)], gathered, *shards)
    (partial,) = call(lent_shard, [((parts, half + channels, width), BF16)], gathered, part, *lent, before, gated, taps)
    partials = exchange(partial, "tp")

    def total(*refs):
        add_parts(side, *refs)

    def tail(*refs):
        mixer_tail(half, *refs)

    (summed,) = call(total, [((slots, width), BF16)], partials)
    (mixed,) = call(tail, [((tokens, width), BF16)], partials, channel_gain[None, :], channel_shift[None, :], mixer_out_weight)
    returned = exchange(summed.reshape(groups, capacity, width), "ep").reshape(slots, width)
    (combined,) = call(combine, [((rows_b, width), BF16)], returned, table)
    return mixed, combined


def solution(mesh):
    in_specs = (
        P("ep", None),
        P(),
        P("tp", None),
        P("tp", None),
        P("tp", None),
        P("tp"),
        P(),
        P(),
        P(None, "tp"),
        P("ep", None),
        P(),
        P("ep", None),
        P("ep", None),
        P("ep", None, "tp"),
        P("ep", None, "tp"),
        P("ep", "tp", None),
    )
    out_specs = (P("ep", "tp"), P("ep", "tp"))

    return jax.shard_map(on_device, mesh=mesh, in_specs=in_specs, out_specs=out_specs, check_vma=False)
```

```python
import math

import jax
import jax.numpy as jnp
from jax import lax
from jax.experimental import pallas as pl
from jax.experimental.pallas import tpu as pltpu
from jax.sharding import PartitionSpec as P


norm_eps = 1e-06
F32 = jnp.float32
BF16 = jnp.bfloat16


def call(body, outs, *operands, far=0):
    near = len(operands) - far
    operands = operands[:near] + tuple(pltpu.with_memory_space_constraint(x, pltpu.HBM) for x in operands[near:])

    def kernel(*refs):
        sources, results = refs[near : near + far], refs[near + far : near + far + len(outs)]
        if not far:
            body(*refs[:near], *results)
            return
        held, sems = refs[near + far + len(outs) : -1], refs[-1]
        copies = [pltpu.make_async_copy(sources[i], held[i], sems.at[i]) for i in range(far)]
        for copy in copies:
            copy.start()
        ready = set()

        def load(i):
            if i not in ready:
                copies[i].wait()
                ready.add(i)
            return held[i]

        body(load, *refs[:near], *results)

    scratch = [pltpu.VMEM(x.shape, x.dtype) for x in operands[near:]]
    return pl.pallas_call(
        kernel,
        out_shape=tuple(jax.ShapeDtypeStruct(s, d) for s, d in outs),
        in_specs=[pl.BlockSpec(memory_space=pltpu.VMEM)] * near + [pl.BlockSpec(memory_space=pltpu.HBM)] * far,
        out_specs=tuple([pl.BlockSpec(memory_space=pltpu.VMEM)] * len(outs)),
        scratch_shapes=scratch + [pltpu.SemaphoreType.DMA((far,))] * (far > 0),
        compiler_params=pltpu.CompilerParams(vmem_limit_bytes=20 * 1024 * 1024),
    )(*operands)


def column_of(row):
    size = row.shape[1]
    at = lax.broadcasted_iota(jnp.int32, (size, size), 0)
    to = lax.broadcasted_iota(jnp.int32, (size, size), 1)
    return jnp.sum(jnp.where(at == to, jnp.broadcast_to(row, (size, size)), 0.0), axis=1, keepdims=True)


def columns_of(row):
    return jnp.transpose(jnp.broadcast_to(row, (8, row.shape[1])))[:, 0:1]


def inv_rms(values):
    return lax.rsqrt(jnp.mean(values * values, axis=-1, keepdims=True) + norm_eps)


def dispatch(groups, capacity, width, load, out_ref, table_ref):
    routes = load(0)[...]
    logits = load(1)[...]
    rows_b = routes.shape[1]
    expert = lax.broadcasted_iota(jnp.int32, (groups, rows_b), 0)
    first = expert == routes[0:1, :]
    second = expert == routes[1:2, :]
    named = jnp.where(first | second, 1.0, 0.0)
    before = lax.broadcasted_iota(jnp.int32, (rows_b, rows_b), 0) < lax.broadcasted_iota(jnp.int32, (rows_b, rows_b), 1)
    earlier = jnp.dot(named.astype(BF16), jnp.where(before, 1.0, 0.0).astype(BF16), preferred_element_type=F32)
    slot = expert.astype(F32) * capacity + earlier
    slot_a = jnp.sum(jnp.where(first, slot, 0.0), axis=0, keepdims=True)
    slot_b = jnp.sum(jnp.where(second, slot, 0.0), axis=0, keepdims=True)
    gap = logits[0:1, :] - logits[1:2, :]
    table_ref[...] = jnp.concatenate([slot_a, slot_b, jax.nn.sigmoid(gap), jax.nn.sigmoid(-gap), jnp.zeros((4, rows_b), F32)], axis=0)
    code = jnp.where(first | second, earlier, -1.0)
    place = lax.broadcasted_iota(jnp.int32, (groups, capacity, rows_b), 1).astype(F32)
    chosen = jnp.where(code[:, None, :] == place, 1.0, 0.0).reshape(groups * capacity, rows_b).astype(BF16)
    gain_ref, rows_ref = load(2), load(3)
    scale = inv_rms(rows_ref[...].astype(F32))
    start = pl.multiple_of(lax.axis_index("tp") * width, width)
    share = rows_ref[:, pl.ds(start, width)].astype(F32)
    normed = (share * scale * gain_ref[:, pl.ds(start, width)]).astype(BF16)
    out_ref[...] = jnp.dot(chosen, normed, preferred_element_type=F32).astype(BF16)


def mixer_front(load, gated_ref, taps_ref):
    taps_ref[...] = jnp.concatenate([load(0)[...], column_of(load(1)[...])], axis=1)
    gain_ref = load(2)
    rows = load(3)[...].astype(F32)
    normed = (rows * inv_rms(rows) * gain_ref[...]).astype(BF16)
    nt = (((1,), (1,)), ((), ()))
    value = lax.dot_general(load(4)[...], normed, nt, preferred_element_type=F32)
    gate = lax.dot_general(load(5)[...], normed, nt, preferred_element_type=F32)
    gated_ref[...] = (value * jax.nn.sigmoid(gate)).astype(BF16)


def row_class(j, side):
    return (j // side + j % side) % 2


def spread_rows(side, arrived_ref, out_ref):
    half = out_ref.shape[1]
    for j in range(out_ref.shape[0]):
        p = row_class(j, side)
        out_ref[j] = arrived_ref[p * half : (p + 1) * half, :]


def convolved(prev_ref, gated_ref, taps_ref):
    width = gated_ref.shape[1]
    taps = taps_ref[...]
    reach = taps.shape[1] - 2
    both = jnp.concatenate([prev_ref[...].astype(F32), gated_ref[...].astype(F32)], axis=1)
    span = both.shape[1]
    total = taps[:, reach + 1 :] + taps[:, reach : reach + 1] * both[:, width:]
    for k in range(reach):
        moved = pltpu.roll(both, reach - k, 1)
        total = total + taps[:, k : k + 1] * moved[:, span - width :]
    return total.astype(BF16)


def shard_part(rows, gate_ref, up_ref, down_ref):
    gate = jnp.dot(rows, gate_ref[0], preferred_element_type=F32)
    up = jnp.dot(rows, up_ref[0], preferred_element_type=F32)
    hidden = (gate * jax.nn.sigmoid(gate) * up).astype(BF16)
    return jnp.dot(hidden, down_ref[0], preferred_element_type=F32)


def own_shard(x_ref, wg_ref, wu_ref, wd_ref, part_ref):
    rows = jnp.concatenate([x_ref[j] for j in range(x_ref.shape[0])], axis=1)
    part_ref[...] = shard_part(rows, wg_ref, wu_ref, wd_ref)


def lent_shard(x_ref, part_ref, wg_ref, wu_ref, wd_ref, prev_ref, gated_ref, taps_ref, out_ref):
    count, slots, width = x_ref.shape
    conv_out = convolved(prev_ref, gated_ref, taps_ref)
    for j in range(count):
        out_ref[j, slots:, :] = conv_out
    rows = jnp.concatenate([x_ref[j] for j in range(count)], axis=1)
    total = (part_ref[...] + shard_part(rows, wg_ref, wu_ref, wd_ref)).astype(BF16)
    for j in range(count):
        out_ref[j, :slots, :] = total[:, j * width : (j + 1) * width]


def mixer_tail(slots, parts_ref, cgain_ref, cshift_ref, wo_ref, out_ref):
    values = jnp.concatenate([parts_ref[j, slots:, :] for j in range(parts_ref.shape[0])], axis=0).astype(F32)
    centered = values - jnp.mean(values, axis=0, keepdims=True)
    variance = jnp.mean(centered * centered, axis=0, keepdims=True)
    shaped = centered * lax.rsqrt(variance + norm_eps) * columns_of(cgain_ref[...]) + columns_of(cshift_ref[...])
    activated = (shaped * jax.nn.sigmoid(shaped)).astype(BF16)
    out_ref[...] = lax.dot_general(activated, wo_ref[...], (((0,), (0,)), ((), ())), preferred_element_type=F32).astype(BF16)


def add_parts(side, capacity, parts_ref, keep_ref, give_ref):
    count, half = parts_ref.shape[0], keep_ref.shape[0]
    core = lax.axis_index("ep") % 2
    block = 2 * capacity
    for p in range(2):
        total = None
        for j in range(count):
            if row_class(j, side) == p:
                term = parts_ref[j, :half, :].astype(F32)
                total = term if total is None else total + term
        total = total.astype(BF16)
        for z in range(half // block):
            even = total[z * block : z * block + capacity]
            odd = total[z * block + capacity : (z + 1) * block]
            at = (p * (half // block) + z) * capacity
            keep_ref[at : at + capacity, :] = jnp.where(core == 0, even, odd)
            give_ref[at : at + capacity, :] = jnp.where(core == 0, odd, even)


def by_chip(capacity, keep_ref, came_ref, out_ref):
    for z in range(out_ref.shape[0]):
        out_ref[z, :capacity, :] = keep_ref[z * capacity : (z + 1) * capacity, :]
        out_ref[z, capacity:, :] = came_ref[z * capacity : (z + 1) * capacity, :]


def combine(capacity, back_ref, table_ref, out_ref):
    slots = back_ref.shape[0]
    table = jnp.transpose(table_ref[...])
    place = lax.broadcasted_iota(jnp.int32, (1, slots), 1)
    turn = jnp.where(place % (2 * capacity) < capacity, capacity, -capacity)
    place = (place + turn * (lax.axis_index("ep") % 2)).astype(F32)
    back = back_ref[...]
    total = None
    for j in range(2):
        pick = jnp.where(table[:, j : j + 1] == place, 1.0, 0.0).astype(BF16)
        term = jnp.dot(pick, back, preferred_element_type=F32) * table[:, 2 + j : 3 + j]
        total = term if total is None else total + term
    out_ref[...] = total.astype(BF16)


def exchange(blocks, axis, members=None):
    return lax.all_to_all(blocks, axis, split_axis=0, concat_axis=0, tiled=True, axis_index_groups=members)


def neighbours(groups, side, along_x):
    pairs = []
    for e in range(groups):
        shift = e % 2

        def other(at):
            return (((at - shift) % side ^ 1) + shift) % side

        for y in range(side):
            for x in range(side):
                to = (y, other(x)) if along_x else (other(y), x)
                pairs.append(((e * side + y) * side + x, (e * side + to[0]) * side + to[1]))
    return pairs


def on_device(
    mixer_input,
    mixer_gain,
    glu_value_weight,
    glu_gate_weight,
    conv_taps,
    conv_bias,
    channel_gain,
    channel_shift,
    mixer_out_weight,
    expert_input,
    expert_gain,
    routes,
    route_logits,
    gate_weight,
    up_weight,
    down_weight,
):
    groups = lax.axis_size("ep")
    parts = lax.axis_size("tp")
    rows_b, features = expert_input.shape
    width = features // parts
    capacity = 3 * rows_b // groups
    slots = groups * capacity
    channels, tokens = glu_value_weight.shape[0], mixer_input.shape[0]

    side = math.isqrt(parts)
    half = slots // 2
    shards = (gate_weight, up_weight, down_weight)


    def front(*refs):
        dispatch(groups, capacity, width, *refs)

    outgoing, table = call(
        front,
        [((slots, width), BF16), ((8, rows_b), F32)],
        routes.T,
        route_logits.T,
        expert_gain[None, :],
        expert_input,
        far=4,
    )
    gated, taps = call(
        mixer_front,
        [((channels, tokens), BF16), ((channels, conv_taps.shape[1] + 1), F32)],
        conv_taps,
        conv_bias[None, :],
        mixer_gain[None, :],
        mixer_input,
        glu_value_weight,
        glu_gate_weight,
        far=6,
    )
    before = lax.ppermute(gated, "ep", [(i, i + 1) for i in range(groups - 1)])
    lent = []
    for w in shards:
        lent.append(lax.ppermute(w, ("ep", "tp"), neighbours(groups, side, True)))
    arrived = exchange(outgoing.reshape(groups, capacity, width), "ep").reshape(slots, width)

    def spread(*refs):
        spread_rows(side, *refs)

    (copies,) = call(spread, [((parts, half, width), BF16)], arrived)
    gathered = exchange(copies, "tp")
    (part,) = call(own_shard, [((half, features), F32)], gathered, *shards)
    (partial,) = call(lent_shard, [((parts, half + channels, width), BF16)], gathered, part, *lent, before, gated, taps)
    partials = exchange(partial, "tp")

    def total(*refs):
        add_parts(side, capacity, *refs)

    def tail(*refs):
        mixer_tail(half, *refs)

    def order(*refs):
        by_chip(capacity, *refs)

    def final(*refs):
        combine(capacity, *refs)

    keep, give = call(total, [((half, width), BF16)] * 2, partials)
    came = lax.ppermute(give, "ep", [(e, e ^ 1) for e in range(groups)])
    (mixed,) = call(tail, [((tokens, width), BF16)], partials, channel_gain[None, :], channel_shift[None, :], mixer_out_weight)
    chips = groups // 2
    (outbound,) = call(order, [((chips, 2 * capacity, width), BF16)], keep, came)
    same_core = [[2 * z + c for z in range(chips)] for c in range(2)]
    returned = exchange(outbound, "ep", same_core).reshape(slots, width)
    (combined,) = call(final, [((rows_b, width), BF16)], returned, table)
    return mixed, combined


def solution(mesh):
    in_specs = (
        P("ep", None),
        P(),
        P("tp", None),
        P("tp", None),
        P("tp", None),
        P("tp"),
        P(),
        P(),
        P(None, "tp"),
        P("ep", None),
        P(),
        P("ep", None),
        P("ep", None),
        P("ep", None, "tp"),
        P("ep", None, "tp"),
        P("ep", "tp", None),
    )
    out_specs = (P("ep", "tp"), P("ep", "tp"))

    return jax.shard_map(on_device, mesh=mesh, in_specs=in_specs, out_specs=out_specs, check_vma=False)
```

```python
import math

import jax
import jax.numpy as jnp
from jax import lax
from jax.experimental import pallas as pl
from jax.experimental.pallas import tpu as pltpu
from jax.sharding import PartitionSpec as P


norm_eps = 1e-06
F32 = jnp.float32
BF16 = jnp.bfloat16


def call(body, outs, *operands, far=0):
    near = len(operands) - far
    operands = operands[:near] + tuple(pltpu.with_memory_space_constraint(x, pltpu.HBM) for x in operands[near:])

    def kernel(*refs):
        sources, results = refs[near : near + far], refs[near + far : near + far + len(outs)]
        if not far:
            body(*refs[:near], *results)
            return
        held, sems = refs[near + far + len(outs) : -1], refs[-1]
        copies = [pltpu.make_async_copy(sources[i], held[i], sems.at[i]) for i in range(far)]
        for copy in copies:
            copy.start()
        ready = set()

        def load(i):
            if i not in ready:
                copies[i].wait()
                ready.add(i)
            return held[i]

        body(load, *refs[:near], *results)

    scratch = [pltpu.VMEM(x.shape, x.dtype) for x in operands[near:]]
    return pl.pallas_call(
        kernel,
        out_shape=tuple(jax.ShapeDtypeStruct(s, d) for s, d in outs),
        in_specs=[pl.BlockSpec(memory_space=pltpu.VMEM)] * near + [pl.BlockSpec(memory_space=pltpu.HBM)] * far,
        out_specs=tuple([pl.BlockSpec(memory_space=pltpu.VMEM)] * len(outs)),
        scratch_shapes=scratch + [pltpu.SemaphoreType.DMA((far,))] * (far > 0),
        compiler_params=pltpu.CompilerParams(vmem_limit_bytes=20 * 1024 * 1024),
    )(*operands)


def column_of(row):
    size = row.shape[1]
    at = lax.broadcasted_iota(jnp.int32, (size, size), 0)
    to = lax.broadcasted_iota(jnp.int32, (size, size), 1)
    return jnp.sum(jnp.where(at == to, jnp.broadcast_to(row, (size, size)), 0.0), axis=1, keepdims=True)


def columns_of(row):
    return jnp.transpose(jnp.broadcast_to(row, (8, row.shape[1])))[:, 0:1]


def inv_rms(values):
    return lax.rsqrt(jnp.mean(values * values, axis=-1, keepdims=True) + norm_eps)


def dispatch(groups, capacity, width, load, out_ref, table_ref):
    routes = load(0)[...]
    logits = load(1)[...]
    rows_b = routes.shape[1]
    expert = lax.broadcasted_iota(jnp.int32, (groups, rows_b), 0)
    first = expert == routes[0:1, :]
    second = expert == routes[1:2, :]
    named = jnp.where(first | second, 1.0, 0.0)
    before = lax.broadcasted_iota(jnp.int32, (rows_b, rows_b), 0) < lax.broadcasted_iota(jnp.int32, (rows_b, rows_b), 1)
    earlier = jnp.dot(named.astype(BF16), jnp.where(before, 1.0, 0.0).astype(BF16), preferred_element_type=F32)
    slot = expert.astype(F32) * capacity + earlier
    slot_a = jnp.sum(jnp.where(first, slot, 0.0), axis=0, keepdims=True)
    slot_b = jnp.sum(jnp.where(second, slot, 0.0), axis=0, keepdims=True)
    gap = logits[0:1, :] - logits[1:2, :]
    table_ref[...] = jnp.concatenate([slot_a, slot_b, jax.nn.sigmoid(gap), jax.nn.sigmoid(-gap), jnp.zeros((4, rows_b), F32)], axis=0)
    code = jnp.where(first | second, earlier, -1.0)
    place = lax.broadcasted_iota(jnp.int32, (groups, capacity, rows_b), 1).astype(F32)
    chosen = jnp.where(code[:, None, :] == place, 1.0, 0.0).reshape(groups * capacity, rows_b).astype(BF16)
    gain_ref, rows_ref = load(2), load(3)
    scale = inv_rms(rows_ref[...].astype(F32))
    start = pl.multiple_of(lax.axis_index("tp") * width, width)
    share = rows_ref[:, pl.ds(start, width)].astype(F32)
    normed = (share * scale * gain_ref[:, pl.ds(start, width)]).astype(BF16)
    out_ref[...] = jnp.dot(chosen, normed, preferred_element_type=F32).astype(BF16)


def mixer_front(load, gated_ref, taps_ref):
    taps_ref[...] = jnp.concatenate([load(0)[...], column_of(load(1)[...])], axis=1)
    gain_ref = load(2)
    rows = load(3)[...].astype(F32)
    normed = (rows * inv_rms(rows) * gain_ref[...]).astype(BF16)
    nt = (((1,), (1,)), ((), ()))
    value = lax.dot_general(load(4)[...], normed, nt, preferred_element_type=F32)
    gate = lax.dot_general(load(5)[...], normed, nt, preferred_element_type=F32)
    gated_ref[...] = (value * jax.nn.sigmoid(gate)).astype(BF16)


def row_class(j, side):
    return (j // side + j % side) % 2


def spread_rows(side, arrived_ref, out_ref):
    half = out_ref.shape[1]
    for j in range(out_ref.shape[0]):
        p = row_class(j, side)
        out_ref[j] = arrived_ref[p * half : (p + 1) * half, :]


def convolved(prev_ref, gated_ref, taps_ref):
    width = gated_ref.shape[1]
    taps = taps_ref[...]
    reach = taps.shape[1] - 2
    both = jnp.concatenate([prev_ref[...].astype(F32), gated_ref[...].astype(F32)], axis=1)
    span = both.shape[1]
    total = taps[:, reach + 1 :] + taps[:, reach : reach + 1] * both[:, width:]
    for k in range(reach):
        moved = pltpu.roll(both, reach - k, 1)
        total = total + taps[:, k : k + 1] * moved[:, span - width :]
    return total.astype(BF16)


def shard_part(rows, gate_ref, up_ref, down_ref):
    gate = jnp.dot(rows, gate_ref[0], preferred_element_type=F32)
    up = jnp.dot(rows, up_ref[0], preferred_element_type=F32)
    hidden = (gate * jax.nn.sigmoid(gate) * up).astype(BF16)
    return jnp.dot(hidden, down_ref[0], preferred_element_type=F32)


def own_shard(x_ref, wg_ref, wu_ref, wd_ref, part_ref):
    rows = jnp.concatenate([x_ref[j] for j in range(x_ref.shape[0])], axis=1)
    part_ref[...] = shard_part(rows, wg_ref, wu_ref, wd_ref)


def lent_shard(x_ref, part_ref, wg_ref, wu_ref, wd_ref, prev_ref, gated_ref, taps_ref, out_ref):
    count, slots, width = x_ref.shape
    conv_out = convolved(prev_ref, gated_ref, taps_ref)
    for j in range(count):
        out_ref[j, slots:, :] = conv_out
    rows = jnp.concatenate([x_ref[j] for j in range(count)], axis=1)
    total = (part_ref[...] + shard_part(rows, wg_ref, wu_ref, wd_ref)).astype(BF16)
    for j in range(count):
        out_ref[j, :slots, :] = total[:, j * width : (j + 1) * width]


def mixer_tail(slots, parts_ref, cgain_ref, cshift_ref, wo_ref, out_ref):
    values = jnp.concatenate([parts_ref[j, slots:, :] for j in range(parts_ref.shape[0])], axis=0).astype(F32)
    centered = values - jnp.mean(values, axis=0, keepdims=True)
    variance = jnp.mean(centered * centered, axis=0, keepdims=True)
    shaped = centered * lax.rsqrt(variance + norm_eps) * columns_of(cgain_ref[...]) + columns_of(cshift_ref[...])
    activated = (shaped * jax.nn.sigmoid(shaped)).astype(BF16)
    out_ref[...] = lax.dot_general(activated, wo_ref[...], (((0,), (0,)), ((), ())), preferred_element_type=F32).astype(BF16)


def add_parts(side, capacity, parts_ref, keep_ref, give_ref):
    count, half = parts_ref.shape[0], keep_ref.shape[0]
    core = lax.axis_index("ep") % 2
    block = 2 * capacity
    for p in range(2):
        total = None
        for j in range(count):
            if row_class(j, side) == p:
                term = parts_ref[j, :half, :].astype(F32)
                total = term if total is None else total + term
        total = total.astype(BF16)
        for z in range(half // block):
            even = total[z * block : z * block + capacity]
            odd = total[z * block + capacity : (z + 1) * block]
            at = (p * (half // block) + z) * capacity
            keep_ref[at : at + capacity, :] = jnp.where(core == 0, even, odd)
            give_ref[at : at + capacity, :] = jnp.where(core == 0, odd, even)


def by_chip(capacity, keep_ref, came_ref, out_ref):
    for z in range(out_ref.shape[0]):
        out_ref[z, :capacity, :] = keep_ref[z * capacity : (z + 1) * capacity, :]
        out_ref[z, capacity:, :] = came_ref[z * capacity : (z + 1) * capacity, :]


def combine(capacity, back_ref, table_ref, out_ref):
    rows_b = out_ref.shape[0]
    slots = back_ref.shape[0]
    table = jnp.transpose(table_ref[...])
    place = lax.broadcasted_iota(jnp.int32, (1, slots), 1)
    turn = jnp.where(place % (2 * capacity) < capacity, capacity, -capacity)
    place = (place + turn * (lax.axis_index("ep") % 2)).astype(F32)
    picks = jnp.concatenate([jnp.where(table[:, j : j + 1] == place, 1.0, 0.0).astype(BF16) for j in range(2)], axis=0)
    rows = jnp.dot(picks, back_ref[...], preferred_element_type=F32)
    total = rows[:rows_b] * table[:, 2:3] + rows[rows_b:] * table[:, 3:4]
    out_ref[...] = total.astype(BF16)


def exchange(blocks, axis, members=None):
    return lax.all_to_all(blocks, axis, split_axis=0, concat_axis=0, tiled=True, axis_index_groups=members)


def neighbours(groups, side, along_x):
    pairs = []
    for e in range(groups):
        shift = e % 2

        def other(at):
            return (((at - shift) % side ^ 1) + shift) % side

        for y in range(side):
            for x in range(side):
                to = (y, other(x)) if along_x else (other(y), x)
                pairs.append(((e * side + y) * side + x, (e * side + to[0]) * side + to[1]))
    return pairs


def on_device(
    mixer_input,
    mixer_gain,
    glu_value_weight,
    glu_gate_weight,
    conv_taps,
    conv_bias,
    channel_gain,
    channel_shift,
    mixer_out_weight,
    expert_input,
    expert_gain,
    routes,
    route_logits,
    gate_weight,
    up_weight,
    down_weight,
):
    groups = lax.axis_size("ep")
    parts = lax.axis_size("tp")
    rows_b, features = expert_input.shape
    width = features // parts
    capacity = 3 * rows_b // groups
    slots = groups * capacity
    channels, tokens = glu_value_weight.shape[0], mixer_input.shape[0]

    side = math.isqrt(parts)
    half = slots // 2
    shards = (gate_weight, up_weight, down_weight)


    def front(*refs):
        dispatch(groups, capacity, width, *refs)

    outgoing, table = call(
        front,
        [((slots, width), BF16), ((8, rows_b), F32)],
        routes.T,
        route_logits.T,
        expert_gain[None, :],
        expert_input,
        far=4,
    )
    gated, taps = call(
        mixer_front,
        [((channels, tokens), BF16), ((channels, conv_taps.shape[1] + 1), F32)],
        conv_taps,
        conv_bias[None, :],
        mixer_gain[None, :],
        mixer_input,
        glu_value_weight,
        glu_gate_weight,
        far=6,
    )
    before = lax.ppermute(gated, "ep", [(i, i + 1) for i in range(groups - 1)])
    lent = []
    for w in shards:
        lent.append(lax.ppermute(w, ("ep", "tp"), neighbours(groups, side, True)))
    arrived = exchange(outgoing.reshape(groups, capacity, width), "ep").reshape(slots, width)

    def spread(*refs):
        spread_rows(side, *refs)

    (copies,) = call(spread, [((parts, half, width), BF16)], arrived)
    gathered = exchange(copies, "tp")
    (part,) = call(own_shard, [((half, features), F32)], gathered, *shards)
    (partial,) = call(lent_shard, [((parts, half + channels, width), BF16)], gathered, part, *lent, before, gated, taps)
    partials = exchange(partial, "tp")

    def total(*refs):
        add_parts(side, capacity, *refs)

    def tail(*refs):
        mixer_tail(half, *refs)

    def order(*refs):
        by_chip(capacity, *refs)

    def final(*refs):
        combine(capacity, *refs)

    keep, give = call(total, [((half, width), BF16)] * 2, partials)
    came = lax.ppermute(give, "ep", [(e, e ^ 1) for e in range(groups)])
    (mixed,) = call(tail, [((tokens, width), BF16)], partials, channel_gain[None, :], channel_shift[None, :], mixer_out_weight)
    chips = groups // 2
    (outbound,) = call(order, [((chips, 2 * capacity, width), BF16)], keep, came)
    same_core = [[2 * z + c for z in range(chips)] for c in range(2)]
    returned = exchange(outbound, "ep", same_core).reshape(slots, width)
    (combined,) = call(final, [((rows_b, width), BF16)], returned, table)
    return mixed, combined


def solution(mesh):
    in_specs = (
        P("ep", None),
        P(),
        P("tp", None),
        P("tp", None),
        P("tp", None),
        P("tp"),
        P(),
        P(),
        P(None, "tp"),
        P("ep", None),
        P(),
        P("ep", None),
        P("ep", None),
        P("ep", None, "tp"),
        P("ep", None, "tp"),
        P("ep", "tp", None),
    )
    out_specs = (P("ep", "tp"), P("ep", "tp"))

    return jax.shard_map(on_device, mesh=mesh, in_specs=in_specs, out_specs=out_specs, check_vma=False)
```
